32 devices in a mesh: ep: 8 (over z, x), tp: 4 (over y, core).
Axes of the slice: x: 2, y: 2, z: 4, core: 2. Of those that a mesh axis runs over, the one named last changes fastest.
Arguments:
- conv_gate: bfloat16 [4096, 2048], P('ep', 'tp'), may hold values from -6 to 6
- conv_in_gate: bfloat16 [4096, 2048], P('ep', 'tp'), may hold values from -6 to 6
- conv_value: bfloat16 [4096, 2048], P('ep', 'tp'), may hold values from -6 to 6
- conv_taps: float32 [3, 2048], P(None, 'tp'), may hold values from -3.5 to 3.5
- mix_out_weight: bfloat16 [2048, 4096], P(None, 'tp'), may hold values from -0.125 to 0.125
- expert_input: bfloat16 [1280, 4096], P('ep', 'tp'), may hold values from -1600 to 1600
- expert_gain: float32 [4096], replicated, may hold values from 0.1 to 1.9
- routes: int32 [1280, 2], P('ep'), may hold values from 0 to 7, all different within a row; in each aligned block of 160 rows (0 to 159, 160 to 319, ...) at most 60 rows name the same one
- group_prob: float32 [1280], P('ep'), may hold values from 0.3 to 1
- pair_logits: float32 [1280, 2], P('ep'), may hold values from -6 to 6
- expert_gate: bfloat16 [8, 4096, 2048], P('ep', None, 'tp'), may hold values from -0.09375 to 0.09375
- expert_up: bfloat16 [8, 4096, 2048], P('ep', None, 'tp'), may hold values from -0.09375 to 0.09375
- expert_down: bfloat16 [8, 2048, 4096], P('ep', None, 'tp'), may hold values from -0.125 to 0.125
Outputs:
- mixed: bfloat16 [4096, 4096], P('ep', 'tp')
- expert_output: bfloat16 [1280, 4096], P('ep', 'tp')
The draws below stay inside these ranges and needn't reach their ends.
Inputs may be any that keep to these rules, and one draw needn't show every extreme that they name: `routes`: in the 160 rows of one index of ep no expert is named by more than 60 rows, a bound that some block reaches; each row names 2 different experts.
All inputs are finite; a program needn't handle non-finite values.
Results may differ from the reference program's by a relative error of at most 0.0071.
Values may be sent and summed in bfloat16 or wider, within the bound.
A program may use at most 64 MiB of HBM per device.

```python
import math
import jax
import jax.numpy as jnp
import numpy as np
from jax import lax

D = 4096
CONV_W = 2048
KERNEL = 3
EXPERT_FF = 2048
TOP = 2
TOK_B_DEV = 160
EXPERTS = 8
CAP = 60
TOK_A = 4096
TOK_B = 1280
N_EP = 8


def draw_expert_input(key, part):
    key_base = jax.random.fold_in(key, 11)
    key_row = jax.random.fold_in(key, 12)
    key_col = jax.random.fold_in(key, 13)
    ramp = jnp.arange(D, dtype=jnp.float32) / D
    base = jnp.clip(jax.random.normal(key_base, (TOK_B, D), jnp.float32), -5.0, 5.0)
    slope = jnp.log(3.0)
    row_scale = 10.0 ** jax.random.uniform(key_row, (TOK_B, 1), jnp.float32)
    col_scale = 10.0 ** jax.random.uniform(key_col, (1, D), jnp.float32) * jnp.exp(slope * ramp)[None, :]
    return (base * row_scale * col_scale).astype(jnp.bfloat16)


def block_levels(stream_key, dims, split, least, high):
    def one(axis_at, blocks):
        heights = jax.random.uniform(jax.random.fold_in(jax.random.fold_in(stream_key, 6), axis_at), (blocks,), jnp.float32, least / len(split), high / len(split))
        return jnp.repeat(jnp.exp(heights), dims[axis_at] // blocks).reshape((-1,) + (1,) * (len(dims) - axis_at - 1))

    factor_of = one(*split[0])
    for cut in split[1:]:
        factor_of = factor_of * one(*cut)
    return factor_of


def routed_block(key, own, number, rows, amount, top, bound, skew):
    order = jax.random.permutation(key, amount)
    packed, common = load_shares(amount, rows * top, bound, skew, True), load_shares(amount, rows * top, bound, skew, False)
    places = jnp.arange(amount)

    def named(lengths, rotation):
        used = int((lengths > 0).sum())
        fixed = max(1, used // 4)
        shifted = fixed + (places - fixed + rotation * (used - fixed)) % max(1, amount - fixed)
        return jnp.zeros((amount,), jnp.int32).at[order[jnp.where(places < fixed, places, shifted)]].set(jnp.asarray(lengths, jnp.int32))

    lengths = jnp.where(number % 4 == 0, named(packed, number // 4), named(common, number - number // 4 - 1))
    mixed = jax.random.permutation(jax.random.fold_in(own, 3), amount)
    giver, receiver = mixed[0:amount // 2 * 2:2], mixed[1:amount // 2 * 2:2]
    margin = jnp.minimum(lengths[giver] - 1, bound - lengths[receiver]) // 2
    margin = jnp.where((giver == order[0]) | (receiver == order[0]) | (lengths[receiver] == 0), 0, jnp.maximum(margin, 0))
    shifted = jax.random.randint(jax.random.fold_in(own, 4), (amount // 2,), 0, 1 << 20) % (margin + 1)
    lengths = lengths.at[giver].add(-shifted).at[receiver].add(shifted)
    items = jnp.searchsorted(jnp.cumsum(lengths), jnp.arange(rows * top), side="right").astype(jnp.int32)
    grid = items.reshape(top, rows).T
    grid = grid[jax.random.permutation(jax.random.fold_in(own, 1), rows)]
    rotation = jax.random.randint(jax.random.fold_in(own, 2), (rows, 1), 0, top)
    return jnp.take_along_axis(grid, (jnp.arange(top)[None, :] + rotation) % top, axis=1)


def load_shares(count, total, most, skew, full):
    portions = [(1 << 20) // math.isqrt(rank ** skew) + 1 for rank in range(1, count + 1)]
    largest = most if full else min(most, max(-(-total // count), total * portions[0] // sum(portions)))
    least = 1 if total - largest >= count - 1 else 0
    counts, rest = [largest] + [least] * (count - 1), total - largest - least * (count - 1)
    while rest > 0:
        free = [i for i in range(1, count) if counts[i] < largest] or [i for i in range(1, count) if counts[i] < most]
        pool, budget = sum([portions[i] for i in free]), rest
        for i in free:
            more = min(most - counts[i], max(1, budget * portions[i] // pool), rest)
            counts[i] = counts[i] + more
            rest = rest - more
    return np.array(counts)


def normal_values(key, dims, width, most, shards=(), held_as=jnp.bfloat16):
    array = jax.random.normal(key, dims, jnp.float32) * width
    if len(shards) > 0:
        array = block_levels(key, dims, shards, -0.22, 0.18) * array
    return jnp.clip(array, min=-most, max=most).astype(held_as)


def setup_inputs(seed: int = 0) -> dict:
    arg_keys = jax.random.split(jax.random.key(seed), 14)
    conv_gate = normal_values(arg_keys[0], (TOK_A, CONV_W), 1.0, 6.0, ((0, 8), (1, 4)))
    conv_in_gate = normal_values(arg_keys[1], (TOK_A, CONV_W), 1.0, 6.0, ((0, 8), (1, 4)))
    conv_value = normal_values(arg_keys[2], (TOK_A, CONV_W), 1.0, 6.0, ((0, 8), (1, 4)))
    conv_taps = normal_values(arg_keys[3], (KERNEL, CONV_W), KERNEL ** -0.5, 3.5, ((1, 4),), jnp.float32)
    mix_out_weight = normal_values(arg_keys[4], (CONV_W, D), CONV_W ** -0.5, 0.125, ((1, 4),))
    expert_input = draw_expert_input(jax.random.fold_in(arg_keys[13], 71), 0)
    expert_gain = jnp.clip(1.0 + 0.18 * jax.random.normal(arg_keys[6], (D,), jnp.float32), 0.1, 1.9)
    routes_keys = jax.random.split(jax.random.fold_in(arg_keys[7], 1), TOK_B // TOK_B_DEV)
    routes_turns = jax.random.permutation(jax.random.fold_in(arg_keys[7], 3), TOK_B // TOK_B_DEV)
    routes = jax.vmap(lambda own, number: routed_block(jax.random.fold_in(arg_keys[7], 2), own, number, TOK_B_DEV, EXPERTS, TOP, CAP, 1))(routes_keys, routes_turns).reshape((TOK_B, TOP))
    group_prob = jnp.clip(0.3 + 0.7 * jax.random.uniform(arg_keys[8], (TOK_B,), jnp.float32) ** block_levels(arg_keys[8], (TOK_B,), ((0, 8),), -0.2, 0.2), 0.3, 1.0)
    pair_logits = normal_values(arg_keys[9], (TOK_B, TOP), 1.5, 6.0, ((0, 8),), jnp.float32)
    expert_gate = normal_values(arg_keys[10], (EXPERTS, D, EXPERT_FF), D ** -0.5, 0.09375, ((0, 8), (2, 4)))
    expert_up = normal_values(arg_keys[11], (EXPERTS, D, EXPERT_FF), D ** -0.5, 0.09375, ((0, 8), (2, 4)))
    expert_down = normal_values(arg_keys[12], (EXPERTS, EXPERT_FF, D), EXPERT_FF ** -0.5, 0.125, ((0, 8), (2, 4)))
    return dict(conv_gate=conv_gate, conv_in_gate=conv_in_gate, conv_value=conv_value, conv_taps=conv_taps, mix_out_weight=mix_out_weight, expert_input=expert_input, expert_gain=expert_gain, routes=routes, group_prob=group_prob, pair_logits=pair_logits, expert_gate=expert_gate, expert_up=expert_up, expert_down=expert_down)


EPS = 1e-06

def slot_table(route_block, capacity, expert_count):
    pair_ids = route_block.reshape(-1)
    onehot = (pair_ids[:, None] == jnp.arange(expert_count, dtype=jnp.int32)[None, :]).astype(jnp.int32)
    earlier = jnp.cumsum(onehot, axis=0) - onehot
    within = lax.optimization_barrier(jnp.sum(earlier * onehot, axis=1))
    return (pair_ids * capacity + within).astype(jnp.int32)

def pair_weights(group_prob, pair_logits):
    spread = pair_logits[:, 0] - pair_logits[:, 1]
    return jnp.stack([jax.nn.sigmoid(spread), jax.nn.sigmoid(-spread)], axis=1) * group_prob[:, None]

def expert_rows(item):
    arrived, gate_w, up_w, down_w = item
    gate_sum = jnp.dot(arrived, gate_w, preferred_element_type=jnp.float32)
    up_sum = jnp.dot(arrived, up_w, preferred_element_type=jnp.float32)
    hidden = (jax.nn.silu(gate_sum) * up_sum).astype(jnp.bfloat16)
    return jnp.dot(hidden, down_w, preferred_element_type=jnp.float32).astype(jnp.bfloat16)

def reference(conv_gate, conv_in_gate, conv_value, conv_taps, mix_out_weight, expert_input, expert_gain, routes, group_prob, pair_logits, expert_gate, expert_up, expert_down):
    products = conv_in_gate.astype(jnp.float32) * conv_value.astype(jnp.float32)
    padded = jnp.concatenate([jnp.zeros((KERNEL - 1, CONV_W), jnp.float32), products], axis=0)
    convolved = jnp.zeros_like(products)
    for offset in range(KERNEL):
        convolved = convolved + conv_taps[offset][None, :] * padded[offset:offset + TOK_A]
    mixer_rows = (conv_gate.astype(jnp.float32) * convolved).astype(jnp.bfloat16)
    mixed = jnp.dot(mixer_rows, mix_out_weight, preferred_element_type=jnp.float32).astype(jnp.bfloat16)
    features = expert_input.astype(jnp.float32)
    scale = lax.rsqrt(lax.optimization_barrier(jnp.mean(features * features, axis=1)) + EPS)
    normed = (features * scale[:, None] * expert_gain[None, :]).astype(jnp.bfloat16)
    blocks = routes.reshape(N_EP, TOK_B_DEV, TOP)

    def block_slots(route_block):
        return slot_table(route_block, CAP, EXPERTS)
    slot_index = jax.vmap(block_slots)(blocks)
    pair_row = (jnp.arange(TOK_B_DEV * TOP, dtype=jnp.int32) // TOP).astype(jnp.int32)
    normed_blocks = normed.reshape(N_EP, TOK_B_DEV, D)

    def fill_buffer(rows_block, slots_block):
        return jnp.zeros((EXPERTS * CAP, D), jnp.bfloat16).at[slots_block].set(rows_block[pair_row])
    buffers = jax.vmap(fill_buffer)(normed_blocks, slot_index)
    per_expert = buffers.reshape(N_EP, EXPERTS, CAP, D).transpose(1, 0, 2, 3).reshape(EXPERTS, N_EP * CAP, D)
    results = lax.map(expert_rows, (per_expert, expert_gate, expert_up, expert_down))
    returned = results.reshape(EXPERTS, N_EP, CAP, D).transpose(1, 0, 2, 3).reshape(N_EP, EXPERTS * CAP, D)

    def pick_rows(table, slots_block):
        return table[slots_block]
    picked = jax.vmap(pick_rows)(returned, slot_index).reshape(TOK_B, TOP, D).astype(jnp.float32)
    weights = pair_weights(group_prob, pair_logits)
    expert_output = lax.optimization_barrier(jnp.sum(picked * weights[:, :, None], axis=1)).astype(jnp.bfloat16)
    return (mixed, expert_output)
```

```python
import functools

import jax
import jax.numpy as jnp
from jax import lax
from jax.experimental import pallas as pl
from jax.experimental.pallas import tpu as pltpu
from jax.sharding import PartitionSpec as P

D = 4096


EPS = 1e-06


def shifted(block, axis, distance):
    devices = range(lax.axis_size(axis))
    route = [(i - distance, i) for i in devices if i - distance in devices]
    return lax.ppermute(block, axis, route)


def slot_table(route_block, capacity, expert_count):
    pair_ids = route_block.reshape(-1)
    onehot = (pair_ids[:, None] == jnp.arange(expert_count, dtype=jnp.int32)[None, :]).astype(
        jnp.int32
    )
    earlier = jnp.cumsum(onehot, axis=0) - onehot
    within = jnp.sum(earlier * onehot, axis=1)
    return pair_ids * capacity + within


def pair_weights(group_prob, pair_logits):
    spread = pair_logits[:, 0] - pair_logits[:, 1]
    return (
        jnp.stack([jax.nn.sigmoid(spread), jax.nn.sigmoid(-spread)], axis=1) * group_prob[:, None]
    )


def per_device(
    conv_gate,
    conv_in_gate,
    conv_value,
    conv_taps,
    mix_out_weight,
    expert_input,
    expert_gain,
    routes,
    group_prob,
    pair_logits,
    expert_gate,
    expert_up,
    expert_down,
):
    reach = conv_taps.shape[0] - 1
    token_rows = conv_value.shape[0]
    products = conv_in_gate.astype(jnp.float32) * conv_value.astype(jnp.float32)
    earlier_rows = shifted(products[token_rows - reach :], "ep", 1)
    padded = jnp.concatenate([earlier_rows, products], axis=0)
    convolved = jnp.zeros_like(products)
    for offset in range(reach + 1):
        convolved = convolved + conv_taps[offset][None, :] * padded[offset : offset + token_rows]
    mixer_rows = (conv_gate.astype(jnp.float32) * convolved).astype(jnp.bfloat16)
    mixed = jnp.dot(
        lax.all_gather(mixer_rows, "tp", axis=1, tiled=True),
        mix_out_weight,
        preferred_element_type=jnp.float32,
    ).astype(jnp.bfloat16)
    expert_count = lax.axis_size("ep")
    tok_rows, choose_count = routes.shape
    capacity = 3 * tok_rows * choose_count // (2 * expert_count)
    slot_index = slot_table(routes, capacity, expert_count)
    pair_row = jnp.arange(tok_rows * choose_count, dtype=jnp.int32) // choose_count
    slot_rows = expert_count * capacity
    gate_block = expert_gate[0]
    up_block = expert_up[0]
    down_block = expert_down[0]
    columns = expert_input.shape[1]
    features = expert_input.astype(jnp.float32)
    squares = lax.psum(jnp.sum(features * features, axis=1), "tp")
    scale = lax.rsqrt(squares / D + EPS)
    gain_part = lax.dynamic_slice_in_dim(expert_gain, lax.axis_index("tp") * columns, columns, 0)
    normed = (features * scale[:, None] * gain_part[None, :]).astype(jnp.bfloat16)
    buffer = jnp.zeros((slot_rows, columns), jnp.bfloat16).at[slot_index].set(normed[pair_row])
    arrived = lax.all_to_all(
        buffer.reshape(expert_count, capacity, columns),
        "ep",
        split_axis=0,
        concat_axis=0,
        tiled=True,
    ).reshape(slot_rows, columns)
    shard_piece = lax.all_gather(arrived, "tp", axis=1, tiled=True)
    gate_sum = jnp.dot(shard_piece, gate_block, preferred_element_type=jnp.float32)
    up_sum = jnp.dot(shard_piece, up_block, preferred_element_type=jnp.float32)
    hidden = (jax.nn.silu(gate_sum) * up_sum).astype(jnp.bfloat16)
    results = jnp.dot(
        lax.all_gather(hidden, "tp", axis=1, tiled=True),
        down_block,
        preferred_element_type=jnp.float32,
    ).astype(jnp.bfloat16)
    returned = lax.all_to_all(
        results.reshape(expert_count, capacity, down_block.shape[1]),
        "ep",
        split_axis=0,
        concat_axis=0,
        tiled=True,
    ).reshape(slot_rows, down_block.shape[1])
    picked = (
        returned[slot_index]
        .reshape(tok_rows, choose_count, down_block.shape[1])
        .astype(jnp.float32)
    )
    weights = pair_weights(group_prob, pair_logits)
    expert_output = jnp.sum(picked * weights[:, :, None], axis=1).astype(jnp.bfloat16)
    return (mixed, expert_output)


CHUNKS = 2
CORES = 2
HALVES = 2
MESH = pl.DeviceIdType.MESH


def fused_kernel(
    n,
    cap,
    pitch,
    gate_h,
    ingate_h,
    value_h,
    taps_ref,
    wmix_h,
    x_ref,
    gain_ref,
    routes_ref,
    prob_ref,
    logits_ref,
    lanes_ref,
    wg_h,
    wu_h,
    wd_h,
    mixed_ref,
    out_ref,
    gate_v,
    ingate_v,
    value_v,
    wmix_v,
    wg_v,
    wu_v,
    wd_v,
    halo,
    padded,
    rows_all,
    picks,
    outgoing,
    arrived,
    normed,
    hidden,
    results,
    returned,
    total,
    local_sem,
    halo_send,
    halo_recv,
    xz_send,
    xz_recv,
    xt_send,
    xt_recv,
    h_send,
    h_recv,
    m_send,
    m_recv,
    ret_send,
    ret_recv,
):
    e = lax.axis_index("ep")
    t = lax.axis_index("tp")
    core = lax.rem(t, CORES)
    t_core = t + 1 - 2 * core
    t_far = lax.rem(t + CORES, 2 * CORES)
    t_far_core = lax.rem(t_core + CORES, 2 * CORES)
    tok_b, columns = x_ref.shape
    tok_a, channels = gate_v.shape
    tp = arrived.shape[0]
    width = columns * tp
    ff = wg_v.shape[1]
    chunk_rows = n * pitch // CHUNKS
    per_chunk = n // CHUNKS
    half_rows = tok_a // HALVES
    tail = halo.shape[1]

    loads = [
        pltpu.make_async_copy(ingate_h, ingate_v, local_sem.at[0]),
        pltpu.make_async_copy(value_h, value_v, local_sem.at[1]),
        pltpu.make_async_copy(gate_h, gate_v, local_sem.at[2]),
        pltpu.make_async_copy(wg_h.at[0], wg_v, local_sem.at[3]),
        pltpu.make_async_copy(wu_h.at[0], wu_v, local_sem.at[4]),
        pltpu.make_async_copy(wd_h.at[0], wd_v, local_sem.at[5]),
        pltpu.make_async_copy(wmix_h, wmix_v, local_sem.at[6]),
    ]
    for load in loads:
        load.start()

    low = cap // 16 * 16
    if cap < pitch:
        for k in range(n):
            spare = pl.ds(k * pitch + low, pitch - low)
            for s in range(tp):
                arrived[s, spare, :] = jnp.zeros((pitch - low, columns), jnp.bfloat16)
            returned[spare, :] = jnp.zeros((pitch - low, columns), jnp.bfloat16)

    barrier = pltpu.get_barrier_semaphore()
    for k in range(1, n):
        pl.semaphore_signal(barrier, inc=1, device_id=(e ^ k, t), device_id_type=MESH)
    pl.semaphore_signal(barrier, inc=1, device_id=(e, t_core), device_id_type=MESH)
    pl.semaphore_signal(barrier, inc=1, device_id=(e, t_far), device_id_type=MESH)

    def block(k):
        return pl.ds(k * pitch, cap)

    expert_of = lanes_ref[0:1, :] ^ e
    place_of = lanes_ref[1:2, :]
    first = (routes_ref[:, 0:1] == expert_of).astype(jnp.float32)
    second = (routes_ref[:, 1:2] == expert_of).astype(jnp.float32)
    named = first + second
    earlier = (
        lax.broadcasted_iota(jnp.int32, (tok_b, tok_b), 1)
        < lax.broadcasted_iota(jnp.int32, (tok_b, tok_b), 0)
    ).astype(jnp.float32)
    within = jnp.dot(
        earlier.astype(jnp.bfloat16),
        named.astype(jnp.bfloat16),
        preferred_element_type=jnp.float32,
    )
    here = (within == place_of.astype(jnp.float32)).astype(jnp.float32)
    spread = logits_ref[:, 0:1] - logits_ref[:, 1:2]
    prob = prob_ref[...]
    w_first = prob * jax.nn.sigmoid(spread)
    w_second = prob * jax.nn.sigmoid(-spread)
    pick = named * here
    weighted = (first * w_first + second * w_second) * here
    high = weighted.astype(jnp.bfloat16)
    picks[0] = high
    picks[1] = (weighted - high.astype(jnp.float32)).astype(jnp.bfloat16)
    outgoing[...] = lax.dot_general(
        pick.astype(jnp.bfloat16),
        x_ref[...],
        (((0,), (0,)), ((), ())),
        preferred_element_type=jnp.float32,
    ).astype(jnp.bfloat16)
    arrived[t, 0:pitch, :] = outgoing[0:pitch, :]

    pl.semaphore_wait(barrier, n + 1)

    xz = [None]
    for k in range(1, n):
        xz.append(
            pltpu.make_async_remote_copy(
                src_ref=outgoing.at[block(k)],
                dst_ref=arrived.at[t, block(k)],
                send_sem=xz_send.at[k],
                recv_sem=xz_recv.at[k],
                device_id=(e ^ k, t),
                device_id_type=MESH,
            )
        )
    for k in reversed(range(1, n)):
        xz[k].start()

    sent = []

    def spread_to(ref, sel, sends, recvs, at):
        def copy(s, way, target):
            return pltpu.make_async_remote_copy(
                src_ref=ref.at[s, sel],
                dst_ref=ref.at[s, sel],
                send_sem=sends.at[way, at],
                recv_sem=recvs.at[way, at],
                device_id=(e, target),
                device_id_type=MESH,
            )

        far, near = copy(t, 0, t_far), copy(t, 1, t_core)
        far.start()
        near.start()
        sent.append(far)
        sent.append(near)

        def relay():
            copy(t_far, 0, t_far).wait_recv()
            passed = copy(t_far, 2, t_core)
            passed.start()
            sent.append(passed)

        def finish():
            copy(t_core, 1, t_core).wait_recv()
            copy(t_far_core, 2, t_core).wait_recv()

        return relay, finish

    loads[0].wait()
    loads[1].wait()
    next_e = lax.rem(e + 1, n)
    tails = [
        pltpu.make_async_remote_copy(
            src_ref=source.at[pl.ds(tok_a - tail, tail)],
            dst_ref=halo.at[i],
            send_sem=halo_send.at[i],
            recv_sem=halo_recv.at[i],
            device_id=(next_e, t),
            device_id_type=MESH,
        )
        for i, source in enumerate((ingate_v, value_v))
    ]
    for copy in tails:
        copy.start()
    top = 8
    padded[top:, :] = ingate_v[...].astype(jnp.float32) * value_v[...].astype(jnp.float32)
    for copy in tails:
        copy.wait()
    before = halo[0].astype(jnp.float32) * halo[1].astype(jnp.float32)
    before = jnp.where(e > 0, before, jnp.zeros_like(before))
    padded[0:top, :] = before[tail - top :, :]
    loads[2].wait()
    reach = taps_ref.shape[0] - 1
    for half in range(HALVES):
        base = half * half_rows
        convolved = jnp.zeros((half_rows, channels), jnp.float32)
        for offset in range(reach + 1):
            convolved = (
                convolved
                + taps_ref[offset : offset + 1, :]
                * padded[pl.ds(base + top - reach + offset, half_rows), :]
            )
        rows_all[t, pl.ds(base, half_rows), :] = (
            gate_v[pl.ds(base, half_rows), :].astype(jnp.float32) * convolved
        ).astype(jnp.bfloat16)
    mix = []
    mix.append(spread_to(rows_all, pl.ds(0, half_rows), m_send, m_recv, 0))

    def chunk_of(j):
        return (CHUNKS - 1 - j) * per_chunk

    def forward(j):
        stages = []
        for k in reversed(range(chunk_of(j), chunk_of(j) + per_chunk)):
            if k > 0:
                xz[k].wait_recv()
            stages.append(spread_to(arrived, block(k), xt_send, xt_recv, k))
        return stages

    def complete(stages):
        for relay, _ in stages:
            relay()
        for _, finish in stages:
            finish()

    def mixer(half):
        complete([mix[half]])
        rows = pl.ds(half * half_rows, half_rows)
        part = jnp.dot(
            rows_all[0, rows, :], wmix_v[0:channels, :], preferred_element_type=jnp.float32
        )
        for s in range(1, tp):
            part = part + jnp.dot(
                rows_all[s, rows, :],
                wmix_v[s * channels : (s + 1) * channels, :],
                preferred_element_type=jnp.float32,
            )
        mixed_ref[rows, :] = part.astype(jnp.bfloat16)

    back = {}
    stages = forward(0)
    for j in range(CHUNKS):
        rows = pl.ds(chunk_of(j) * pitch, chunk_rows)
        complete(stages)
        squares = jnp.zeros((chunk_rows, 1), jnp.float32)
        for s in range(tp):
            block_f = arrived[s, rows, :].astype(jnp.float32)
            squares = squares + jnp.sum(block_f * block_f, axis=1, keepdims=True)
        scale = lax.rsqrt(squares / width + EPS)
        for s in range(tp):
            cols = slice(s * columns, (s + 1) * columns)
            normed[:, cols] = (
                arrived[s, rows, :].astype(jnp.float32) * scale * gain_ref[:, cols]
            ).astype(jnp.bfloat16)
        if j == 0:
            loads[3].wait()
            loads[4].wait()
        gate_sum = jnp.dot(normed[...], wg_v[...], preferred_element_type=jnp.float32)
        up_sum = jnp.dot(normed[...], wu_v[...], preferred_element_type=jnp.float32)
        hidden[t, rows, :] = (gate_sum / (1.0 + jnp.exp(-gate_sum)) * up_sum).astype(jnp.bfloat16)
        h_stage = spread_to(hidden, rows, h_send, h_recv, j)
        if j == 0:
            loads[6].wait()
            mixer(0)
        if j + 1 < CHUNKS:
            stages = forward(j + 1)
        else:
            for half in range(1, HALVES):
                mix.append(
                    spread_to(rows_all, pl.ds(half * half_rows, half_rows), m_send, m_recv, half)
                )
        complete([h_stage])
        if j == 0:
            loads[5].wait()
        part = jnp.dot(hidden[0, rows, :], wd_v[0:ff, :], preferred_element_type=jnp.float32)
        for s in range(1, tp):
            part = part + jnp.dot(
                hidden[s, rows, :],
                wd_v[s * ff : (s + 1) * ff, :],
                preferred_element_type=jnp.float32,
            )
        results[rows, :] = part.astype(jnp.bfloat16)
        for k in reversed(range(chunk_of(j), chunk_of(j) + per_chunk)):
            if k > 0:
                back[k] = pltpu.make_async_remote_copy(
                    src_ref=results.at[block(k)],
                    dst_ref=returned.at[block(k)],
                    send_sem=ret_send.at[k],
                    recv_sem=ret_recv.at[k],
                    device_id=(e ^ k, t),
                    device_id_type=MESH,
                )
                back[k].start()
            else:
                returned[0:pitch, :] = results[0:pitch, :]

    for half in range(1, HALVES):
        mixer(half)

    for j in reversed(range(CHUNKS)):
        for k in range(max(1, chunk_of(j)), chunk_of(j) + per_chunk):
            back[k].wait_recv()
        span = slice(chunk_of(j) * pitch, chunk_of(j) * pitch + chunk_rows)
        term = jnp.dot(
            picks[0, :, span], returned[span, :], preferred_element_type=jnp.float32
        ) + jnp.dot(picks[1, :, span], returned[span, :], preferred_element_type=jnp.float32)
        if j == CHUNKS - 1:
            total[...] = term
        else:
            total[...] += term
    out_ref[...] = total[...].astype(jnp.bfloat16)

    for k in range(1, n):
        xz[k].wait_send()
        back[k].wait_send()
    for copy in sent:
        copy.wait_send()


def fused_device(
    conv_gate,
    conv_in_gate,
    conv_value,
    conv_taps,
    mix_out_weight,
    expert_input,
    expert_gain,
    routes,
    group_prob,
    pair_logits,
    expert_gate,
    expert_up,
    expert_down,
):
    n, tp = lax.axis_size("ep"), lax.axis_size("tp")
    tok_b, columns = expert_input.shape
    tok_a, channels = conv_value.shape
    width, ff = expert_gate.shape[1:]
    cap = 3 * tok_b * routes.shape[1] // (2 * n)
    pitch = -(-cap // 16) * 16
    cap = -(-cap // 8) * 8
    slots = n * pitch
    lane = jnp.arange(slots, dtype=jnp.int32)
    lanes = jnp.stack([lane // pitch, lane % pitch])
    chunk_rows = slots // CHUNKS
    tail = 16
    any_spec = pl.BlockSpec(memory_space=pl.ANY)
    vmem = pl.BlockSpec(memory_space=pltpu.VMEM)
    dma = pltpu.SemaphoreType.DMA
    bf16, f32 = jnp.bfloat16, jnp.float32
    return pl.pallas_call(
        functools.partial(fused_kernel, n, cap, pitch),
        out_shape=(
            jax.ShapeDtypeStruct((tok_a, mix_out_weight.shape[1]), bf16),
            jax.ShapeDtypeStruct((tok_b, columns), bf16),
        ),
        in_specs=[
            any_spec, any_spec, any_spec, vmem, any_spec, vmem, vmem, vmem, vmem, vmem, vmem,
            any_spec, any_spec, any_spec,
        ],
        out_specs=(vmem, vmem),
        scratch_shapes=[
            pltpu.VMEM((tok_a, channels), bf16),
            pltpu.VMEM((tok_a, channels), bf16),
            pltpu.VMEM((tok_a, channels), bf16),
            pltpu.VMEM(mix_out_weight.shape, bf16),
            pltpu.VMEM((width, ff), bf16),
            pltpu.VMEM((width, ff), bf16),
            pltpu.VMEM(expert_down.shape[1:], bf16),
            pltpu.VMEM((2, tail, channels), bf16),
            pltpu.VMEM((8 + tok_a, channels), f32),
            pltpu.VMEM((tp, tok_a, channels), bf16),
            pltpu.VMEM((2, tok_b, slots), bf16),
            pltpu.VMEM((slots, columns), bf16),
            pltpu.VMEM((tp, slots, columns), bf16),
            pltpu.VMEM((chunk_rows, width), bf16),
            pltpu.VMEM((tp, slots, ff), bf16),
            pltpu.VMEM((slots, columns), bf16),
            pltpu.VMEM((slots, columns), bf16),
            pltpu.VMEM((tok_b, columns), f32),
            dma((7,)),
            dma((2,)),
            dma((2,)),
            dma((n,)),
            dma((n,)),
            dma((3, n)),
            dma((3, n)),
            dma((3, CHUNKS)),
            dma((3, CHUNKS)),
            dma((3, HALVES)),
            dma((3, HALVES)),
            dma((n,)),
            dma((n,)),
        ],
        compiler_params=pltpu.CompilerParams(
            collective_id=0, has_side_effects=True, vmem_limit_bytes=60 * 1024 * 1024
        ),
    )(
        conv_gate,
        conv_in_gate,
        conv_value,
        conv_taps,
        mix_out_weight,
        expert_input,
        expert_gain.reshape(1, width),
        routes,
        group_prob.reshape(tok_b, 1),
        pair_logits,
        lanes,
        expert_gate,
        expert_up,
        expert_down,
    )


def solution(mesh):
    partners = mesh.shape["ep"]
    fused = mesh.shape["tp"] == 2 * CORES and partners & (partners - 1) == 0
    body = fused_device if fused else per_device
    in_specs = (
        P("ep", "tp"),
        P("ep", "tp"),
        P("ep", "tp"),
        P(None, "tp"),
        P(None, "tp"),
        P("ep", "tp"),
        P(),
        P("ep", None),
        P("ep"),
        P("ep", None),
        P("ep", None, "tp"),
        P("ep", None, "tp"),
        P("ep", None, "tp"),
    )
    out_specs = (P("ep", "tp"), P("ep", "tp"))
    return jax.shard_map(
        body, mesh=mesh, in_specs=in_specs, out_specs=out_specs, check_vma=False
    )
```

```python
import functools

import jax
import jax.numpy as jnp
from jax import lax
from jax.experimental import pallas as pl
from jax.experimental.pallas import tpu as pltpu
from jax.sharding import PartitionSpec as P

D = 4096


EPS = 1e-06


def shifted(block, axis, distance):
    devices = range(lax.axis_size(axis))
    route = [(i - distance, i) for i in devices if i - distance in devices]
    return lax.ppermute(block, axis, route)


def slot_table(route_block, capacity, expert_count):
    pair_ids = route_block.reshape(-1)
    onehot = (pair_ids[:, None] == jnp.arange(expert_count, dtype=jnp.int32)[None, :]).astype(
        jnp.int32
    )
    earlier = jnp.cumsum(onehot, axis=0) - onehot
    within = jnp.sum(earlier * onehot, axis=1)
    return pair_ids * capacity + within


def pair_weights(group_prob, pair_logits):
    spread = pair_logits[:, 0] - pair_logits[:, 1]
    return (
        jnp.stack([jax.nn.sigmoid(spread), jax.nn.sigmoid(-spread)], axis=1) * group_prob[:, None]
    )


def per_device(
    conv_gate,
    conv_in_gate,
    conv_value,
    conv_taps,
    mix_out_weight,
    expert_input,
    expert_gain,
    routes,
    group_prob,
    pair_logits,
    expert_gate,
    expert_up,
    expert_down,
):
    reach = conv_taps.shape[0] - 1
    token_rows = conv_value.shape[0]
    products = conv_in_gate.astype(jnp.float32) * conv_value.astype(jnp.float32)
    earlier_rows = shifted(products[token_rows - reach :], "ep", 1)
    padded = jnp.concatenate([earlier_rows, products], axis=0)
    convolved = jnp.zeros_like(products)
    for offset in range(reach + 1):
        convolved = convolved + conv_taps[offset][None, :] * padded[offset : offset + token_rows]
    mixer_rows = (conv_gate.astype(jnp.float32) * convolved).astype(jnp.bfloat16)
    mixed = jnp.dot(
        lax.all_gather(mixer_rows, "tp", axis=1, tiled=True),
        mix_out_weight,
        preferred_element_type=jnp.float32,
    ).astype(jnp.bfloat16)
    expert_count = lax.axis_size("ep")
    tok_rows, choose_count = routes.shape
    capacity = 3 * tok_rows * choose_count // (2 * expert_count)
    slot_index = slot_table(routes, capacity, expert_count)
    pair_row = jnp.arange(tok_rows * choose_count, dtype=jnp.int32) // choose_count
    slot_rows = expert_count * capacity
    gate_block = expert_gate[0]
    up_block = expert_up[0]
    down_block = expert_down[0]
    columns = expert_input.shape[1]
    features = expert_input.astype(jnp.float32)
    squares = lax.psum(jnp.sum(features * features, axis=1), "tp")
    scale = lax.rsqrt(squares / D + EPS)
    gain_part = lax.dynamic_slice_in_dim(expert_gain, lax.axis_index("tp") * columns, columns, 0)
    normed = (features * scale[:, None] * gain_part[None, :]).astype(jnp.bfloat16)
    buffer = jnp.zeros((slot_rows, columns), jnp.bfloat16).at[slot_index].set(normed[pair_row])
    arrived = lax.all_to_all(
        buffer.reshape(expert_count, capacity, columns),
        "ep",
        split_axis=0,
        concat_axis=0,
        tiled=True,
    ).reshape(slot_rows, columns)
    shard_piece = lax.all_gather(arrived, "tp", axis=1, tiled=True)
    gate_sum = jnp.dot(shard_piece, gate_block, preferred_element_type=jnp.float32)
    up_sum = jnp.dot(shard_piece, up_block, preferred_element_type=jnp.float32)
    hidden = (jax.nn.silu(gate_sum) * up_sum).astype(jnp.bfloat16)
    results = jnp.dot(
        lax.all_gather(hidden, "tp", axis=1, tiled=True),
        down_block,
        preferred_element_type=jnp.float32,
    ).astype(jnp.bfloat16)
    returned = lax.all_to_all(
        results.reshape(expert_count, capacity, down_block.shape[1]),
        "ep",
        split_axis=0,
        concat_axis=0,
        tiled=True,
    ).reshape(slot_rows, down_block.shape[1])
    picked = (
        returned[slot_index]
        .reshape(tok_rows, choose_count, down_block.shape[1])
        .astype(jnp.float32)
    )
    weights = pair_weights(group_prob, pair_logits)
    expert_output = jnp.sum(picked * weights[:, :, None], axis=1).astype(jnp.bfloat16)
    return (mixed, expert_output)


CHUNKS = 2
CORES = 2
HALVES = 2
EARLY = 1
MESH = pl.DeviceIdType.MESH


def fused_kernel(
    n,
    cap,
    pitch,
    gate_h,
    ingate_h,
    value_h,
    taps_ref,
    wmix_h,
    x_ref,
    gain_ref,
    routes_ref,
    prob_ref,
    logits_ref,
    wg_h,
    wu_h,
    wd_h,
    mixed_ref,
    out_ref,
    gate_v,
    ingate_v,
    value_v,
    wmix_v,
    wg_v,
    wu_v,
    wd_v,
    halo,
    padded,
    rows_all,
    picks,
    outgoing,
    arrived,
    normed,
    hidden,
    results,
    returned,
    total,
    local_sem,
    halo_send,
    halo_recv,
    xz_send,
    xz_recv,
    xt_send,
    xt_recv,
    h_send,
    h_recv,
    m_send,
    m_recv,
    ret_send,
    ret_recv,
):
    e = lax.axis_index("ep")
    t = lax.axis_index("tp")
    core = lax.rem(t, CORES)
    t_core = t + 1 - 2 * core
    t_far = lax.rem(t + CORES, 2 * CORES)
    t_far_core = lax.rem(t_core + CORES, 2 * CORES)
    tok_b, columns = x_ref.shape
    tok_a, channels = gate_v.shape
    tp = arrived.shape[0]
    width = columns * tp
    ff = wg_v.shape[1]
    chunk_rows = n * pitch // CHUNKS
    per_chunk = n // CHUNKS
    half_rows = tok_a // HALVES
    tail = halo.shape[1]

    loads = [
        pltpu.make_async_copy(ingate_h, ingate_v, local_sem.at[0]),
        pltpu.make_async_copy(value_h, value_v, local_sem.at[1]),
        pltpu.make_async_copy(gate_h, gate_v, local_sem.at[2]),
        pltpu.make_async_copy(wg_h.at[0], wg_v, local_sem.at[3]),
        pltpu.make_async_copy(wu_h.at[0], wu_v, local_sem.at[4]),
        pltpu.make_async_copy(wd_h.at[0], wd_v, local_sem.at[5]),
        pltpu.make_async_copy(wmix_h, wmix_v, local_sem.at[6]),
    ]
    for load in loads:
        load.start()

    low = cap // 16 * 16
    if cap < pitch:
        for k in range(n):
            spare = pl.ds(k * pitch + low, pitch - low)
            for s in range(tp):
                arrived[s, spare, :] = jnp.zeros((pitch - low, columns), jnp.bfloat16)
            returned[spare, :] = jnp.zeros((pitch - low, columns), jnp.bfloat16)

    barrier = pltpu.get_barrier_semaphore()
    for k in range(1, n):
        pl.semaphore_signal(barrier, inc=1, device_id=(e ^ k, t), device_id_type=MESH)
    pl.semaphore_signal(barrier, inc=1, device_id=(e, t_core), device_id_type=MESH)
    pl.semaphore_signal(barrier, inc=1, device_id=(e, t_far), device_id_type=MESH)

    def block(k):
        return pl.ds(k * pitch, cap)

    lane = lax.broadcasted_iota(jnp.int32, (1, n * pitch), 1)
    partner = jnp.zeros_like(lane)
    for k in range(1, n):
        partner = partner + (lane >= k * pitch).astype(jnp.int32)
    expert_of = (partner ^ e).astype(jnp.float32)
    place_of = lane - partner * pitch
    row_at = lax.broadcasted_iota(jnp.int32, (tok_b, tok_b), 0)
    lane_at = lax.broadcasted_iota(jnp.int32, (tok_b, tok_b), 1)

    def column(row):
        return jnp.sum(jnp.where(row_at == lane_at, row, 0.0), axis=1, keepdims=True)

    routes_f = routes_ref[...].astype(jnp.float32)
    first = (column(routes_f[0:1, :]) == expert_of).astype(jnp.float32)
    second = (column(routes_f[1:2, :]) == expert_of).astype(jnp.float32)
    named = first + second
    earlier = (lane_at < row_at).astype(jnp.float32)
    within = jnp.dot(
        earlier.astype(jnp.bfloat16),
        named.astype(jnp.bfloat16),
        preferred_element_type=jnp.float32,
    )
    here = (within == place_of.astype(jnp.float32)).astype(jnp.float32)
    spread = logits_ref[0:1, :] - logits_ref[1:2, :]
    prob = prob_ref[...]
    w_first = column(prob * jax.nn.sigmoid(spread))
    w_second = column(prob * jax.nn.sigmoid(-spread))
    pick = named * here
    weighted = (first * w_first + second * w_second) * here
    high = weighted.astype(jnp.bfloat16)
    picks[0] = high
    picks[1] = (weighted - high.astype(jnp.float32)).astype(jnp.bfloat16)
    outgoing[...] = lax.dot_general(
        pick.astype(jnp.bfloat16),
        x_ref[...],
        (((0,), (0,)), ((), ())),
        preferred_element_type=jnp.float32,
    ).astype(jnp.bfloat16)
    arrived[t, 0:pitch, :] = outgoing[0:pitch, :]

    pl.semaphore_wait(barrier, n + 1)

    loads[0].wait()
    loads[1].wait()
    next_e = lax.rem(e + 1, n)
    tails = [
        pltpu.make_async_remote_copy(
            src_ref=source.at[pl.ds(tok_a - tail, tail)],
            dst_ref=halo.at[i],
            send_sem=halo_send.at[i],
            recv_sem=halo_recv.at[i],
            device_id=(next_e, t),
            device_id_type=MESH,
        )
        for i, source in enumerate((ingate_v, value_v))
    ]
    for copy in tails:
        copy.start()

    xz = [None]
    for k in range(1, n):
        xz.append(
            pltpu.make_async_remote_copy(
                src_ref=outgoing.at[block(k)],
                dst_ref=arrived.at[t, block(k)],
                send_sem=xz_send.at[k],
                recv_sem=xz_recv.at[k],
                device_id=(e ^ k, t),
                device_id_type=MESH,
            )
        )
    for k in reversed(range(1, n)):
        xz[k].start()

    sent = []

    def spread_to(ref, sel, sends, recvs, at):
        def copy(s, way, target):
            return pltpu.make_async_remote_copy(
                src_ref=ref.at[s, sel],
                dst_ref=ref.at[s, sel],
                send_sem=sends.at[way, at],
                recv_sem=recvs.at[way, at],
                device_id=(e, target),
                device_id_type=MESH,
            )

        far, near = copy(t, 0, t_far), copy(t, 1, t_core)
        far.start()
        near.start()
        sent.append(far)
        sent.append(near)

        def relay():
            copy(t_far, 0, t_far).wait_recv()
            passed = copy(t_far, 2, t_core)
            passed.start()
            sent.append(passed)

        def finish():
            copy(t_core, 1, t_core).wait_recv()
            copy(t_far_core, 2, t_core).wait_recv()

        return relay, finish

    top = 8
    padded[top:, :] = ingate_v[...].astype(jnp.float32) * value_v[...].astype(jnp.float32)
    for copy in tails:
        copy.wait()
    before = halo[0].astype(jnp.float32) * halo[1].astype(jnp.float32)
    before = jnp.where(e > 0, before, jnp.zeros_like(before))
    padded[0:top, :] = before[tail - top :, :]
    loads[2].wait()
    reach = taps_ref.shape[0] - 1
    for half in range(HALVES):
        base = half * half_rows
        convolved = jnp.zeros((half_rows, channels), jnp.float32)
        for offset in range(reach + 1):
            convolved = (
                convolved
                + taps_ref[offset : offset + 1, :]
                * padded[pl.ds(base + top - reach + offset, half_rows), :]
            )
        rows_all[t, pl.ds(base, half_rows), :] = (
            gate_v[pl.ds(base, half_rows), :].astype(jnp.float32) * convolved
        ).astype(jnp.bfloat16)
    mix = []

    def spread_rows(half):
        mix.append(spread_to(rows_all, pl.ds(half * half_rows, half_rows), m_send, m_recv, half))

    for half in range(EARLY):
        spread_rows(half)

    def chunk_of(j):
        return (CHUNKS - 1 - j) * per_chunk

    def forward(k):
        if k > 0:
            xz[k].wait_recv()
        return spread_to(arrived, block(k), xt_send, xt_recv, k)

    def partners(j):
        return list(reversed(range(chunk_of(j), chunk_of(j) + per_chunk)))

    def complete(stages):
        for relay, _ in stages:
            relay()
        for _, finish in stages:
            finish()

    def mixer(half):
        complete([mix[half]])
        rows = pl.ds(half * half_rows, half_rows)
        part = jnp.dot(
            rows_all[0, rows, :], wmix_v[0:channels, :], preferred_element_type=jnp.float32
        )
        for s in range(1, tp):
            part = part + jnp.dot(
                rows_all[s, rows, :],
                wmix_v[s * channels : (s + 1) * channels, :],
                preferred_element_type=jnp.float32,
            )
        mixed_ref[rows, :] = part.astype(jnp.bfloat16)

    back = {}
    order = partners(0)
    stages = [forward(k) for k in order[: per_chunk // 2]]
    loads[6].wait()
    for half in range(EARLY):
        mixer(half)
    stages += [forward(k) for k in order[per_chunk // 2 :]]
    for j in range(CHUNKS):
        rows = pl.ds(chunk_of(j) * pitch, chunk_rows)
        complete(stages)
        squares = jnp.zeros((chunk_rows, 1), jnp.float32)
        for s in range(tp):
            block_f = arrived[s, rows, :].astype(jnp.float32)
            squares = squares + jnp.sum(block_f * block_f, axis=1, keepdims=True)
        scale = lax.rsqrt(squares / width + EPS)
        for s in range(tp):
            cols = slice(s * columns, (s + 1) * columns)
            normed[:, cols] = (
                arrived[s, rows, :].astype(jnp.float32) * scale * gain_ref[:, cols]
            ).astype(jnp.bfloat16)
        if j == 0:
            loads[3].wait()
            loads[4].wait()
        gate_sum = jnp.dot(normed[...], wg_v[...], preferred_element_type=jnp.float32)
        up_sum = jnp.dot(normed[...], wu_v[...], preferred_element_type=jnp.float32)
        hidden[t, rows, :] = (gate_sum / (1.0 + jnp.exp(-gate_sum)) * up_sum).astype(jnp.bfloat16)
        h_stage = spread_to(hidden, rows, h_send, h_recv, j)
        if j + 1 < CHUNKS:
            stages = [forward(k) for k in partners(j + 1)]
        else:
            for half in range(EARLY, HALVES):
                spread_rows(half)
        complete([h_stage])
        if j == 0:
            loads[5].wait()
        part = jnp.dot(hidden[0, rows, :], wd_v[0:ff, :], preferred_element_type=jnp.float32)
        for s in range(1, tp):
            part = part + jnp.dot(
                hidden[s, rows, :],
                wd_v[s * ff : (s + 1) * ff, :],
                preferred_element_type=jnp.float32,
            )
        results[rows, :] = part.astype(jnp.bfloat16)
        for k in reversed(range(chunk_of(j), chunk_of(j) + per_chunk)):
            if k > 0:
                back[k] = pltpu.make_async_remote_copy(
                    src_ref=results.at[block(k)],
                    dst_ref=returned.at[block(k)],
                    send_sem=ret_send.at[k],
                    recv_sem=ret_recv.at[k],
                    device_id=(e ^ k, t),
                    device_id_type=MESH,
                )
                back[k].start()
            else:
                returned[0:pitch, :] = results[0:pitch, :]

    for half in range(EARLY, HALVES):
        mixer(half)

    for j in reversed(range(CHUNKS)):
        for k in range(max(1, chunk_of(j)), chunk_of(j) + per_chunk):
            back[k].wait_recv()
        span = slice(chunk_of(j) * pitch, chunk_of(j) * pitch + chunk_rows)
        term = jnp.dot(
            picks[0, :, span], returned[span, :], preferred_element_type=jnp.float32
        ) + jnp.dot(picks[1, :, span], returned[span, :], preferred_element_type=jnp.float32)
        if j == CHUNKS - 1:
            total[...] = term
        else:
            total[...] += term
    out_ref[...] = total[...].astype(jnp.bfloat16)

    for k in range(1, n):
        xz[k].wait_send()
        back[k].wait_send()
    for copy in sent:
        copy.wait_send()


def hand_over(mixed_in, out_in, mixed_ref, out_ref):
    mixed_ref[...] = mixed_in[...]
    out_ref[...] = out_in[...]


def fused_device(
    conv_gate,
    conv_in_gate,
    conv_value,
    conv_taps,
    mix_out_weight,
    expert_input,
    expert_gain,
    routes,
    group_prob,
    pair_logits,
    expert_gate,
    expert_up,
    expert_down,
):
    n, tp = lax.axis_size("ep"), lax.axis_size("tp")
    tok_b, columns = expert_input.shape
    tok_a, channels = conv_value.shape
    width, ff = expert_gate.shape[1:]
    cap = 3 * tok_b * routes.shape[1] // (2 * n)
    pitch = -(-cap // 16) * 16
    cap = -(-cap // 8) * 8
    slots = n * pitch
    chunk_rows = slots // CHUNKS
    tail = 16
    any_spec = pl.BlockSpec(memory_space=pl.ANY)
    vmem = pl.BlockSpec(memory_space=pltpu.VMEM)
    dma = pltpu.SemaphoreType.DMA
    bf16, f32 = jnp.bfloat16, jnp.float32
    outputs = pl.pallas_call(
        functools.partial(fused_kernel, n, cap, pitch),
        out_shape=(
            jax.ShapeDtypeStruct((tok_a, mix_out_weight.shape[1]), bf16),
            jax.ShapeDtypeStruct((tok_b, columns), bf16),
        ),
        in_specs=[
            any_spec, any_spec, any_spec, vmem, any_spec, vmem, vmem, vmem, vmem, vmem,
            any_spec, any_spec, any_spec,
        ],
        out_specs=(vmem, vmem),
        scratch_shapes=[
            pltpu.VMEM((tok_a, channels), bf16),
            pltpu.VMEM((tok_a, channels), bf16),
            pltpu.VMEM((tok_a, channels), bf16),
            pltpu.VMEM(mix_out_weight.shape, bf16),
            pltpu.VMEM((width, ff), bf16),
            pltpu.VMEM((width, ff), bf16),
            pltpu.VMEM(expert_down.shape[1:], bf16),
            pltpu.VMEM((2, tail, channels), bf16),
            pltpu.VMEM((8 + tok_a, channels), f32),
            pltpu.VMEM((tp, tok_a, channels), bf16),
            pltpu.VMEM((2, tok_b, slots), bf16),
            pltpu.VMEM((slots, columns), bf16),
            pltpu.VMEM((tp, slots, columns), bf16),
            pltpu.VMEM((chunk_rows, width), bf16),
            pltpu.VMEM((tp, slots, ff), bf16),
            pltpu.VMEM((slots, columns), bf16),
            pltpu.VMEM((slots, columns), bf16),
            pltpu.VMEM((tok_b, columns), f32),
            dma((7,)),
            dma((2,)),
            dma((2,)),
            dma((n,)),
            dma((n,)),
            dma((3, n)),
            dma((3, n)),
            dma((3, CHUNKS)),
            dma((3, CHUNKS)),
            dma((3, HALVES)),
            dma((3, HALVES)),
            dma((n,)),
            dma((n,)),
        ],
        compiler_params=pltpu.CompilerParams(
            collective_id=0, has_side_effects=True, vmem_limit_bytes=60 * 1024 * 1024
        ),
    )(
        conv_gate,
        conv_in_gate,
        conv_value,
        conv_taps,
        mix_out_weight,
        expert_input,
        expert_gain.reshape(1, width),
        routes.T,
        group_prob.reshape(1, tok_b),
        pair_logits.T,
        expert_gate,
        expert_up,
        expert_down,
    )
    return pl.pallas_call(
        hand_over,
        out_shape=tuple(jax.ShapeDtypeStruct(o.shape, o.dtype) for o in outputs),
        in_specs=[vmem, vmem],
        out_specs=(vmem, vmem),
    )(*outputs)


def solution(mesh):
    partners = mesh.shape["ep"]
    fused = mesh.shape["tp"] == 2 * CORES and partners & (partners - 1) == 0
    body = fused_device if fused else per_device
    in_specs = (
        P("ep", "tp"),
        P("ep", "tp"),
        P("ep", "tp"),
        P(None, "tp"),
        P(None, "tp"),
        P("ep", "tp"),
        P(),
        P("ep", None),
        P("ep"),
        P("ep", None),
        P("ep", None, "tp"),
        P("ep", None, "tp"),
        P("ep", None, "tp"),
    )
    out_specs = (P("ep", "tp"), P("ep", "tp"))
    return jax.shard_map(
        body, mesh=mesh, in_specs=in_specs, out_specs=out_specs, check_vma=False
    )
```
